32 devices in a mesh: grp: 2 (over y), ep: 4 (over z), tp: 4 (over x, core).
Axes of the slice: x: 2, y: 2, z: 4, core: 2. Of those that a mesh axis runs over, the one named last changes fastest.
Arguments:
- tokens: bfloat16 [512, 4096], P(('grp', 'ep'), 'tp'), parts along dimension 0, may hold values from -27 to 27
- group_choice: int32 [512], P(('grp', 'ep')), parts along dimension 0, may hold values from 0 to 1, as said below
- member_choice: int32 [512, 2], P(('grp', 'ep')), parts along dimension 0, may hold values from 0 to 1, as said below
- group_prob: float32 [512], P(('grp', 'ep')), parts along dimension 0, may hold values from 0.3 to 1
- member_score: float32 [512, 2], P(('grp', 'ep')), parts along dimension 0, may hold values from -4 to 4
- norm_gain: float32 [4096], P('tp'), may hold values from 0.1 to 1.9
- w_gate: bfloat16 [4, 4096, 1024], P('ep', 'tp'), may hold values from -0.09375 to 0.09375
- w_up: bfloat16 [4, 4096, 1024], P('ep', 'tp'), may hold values from -0.09375 to 0.09375
- w_down: bfloat16 [4, 1024, 4096], P('ep', None, 'tp'), may hold values from -0.1875 to 0.1875
- final_gain: float32 [4096], P('tp'), may hold values from 0.1 to 1.9
Outputs:
- mixed: bfloat16 [512, 4096], P(('grp', 'ep'), 'tp'), parts along dimension 0
The draws below stay inside these ranges and needn't reach their ends.
There are 2 independent parts, one for each index of `grp`. The reference program is written for one: setup_inputs(seed, part) draws one part's arguments, and reference() takes and returns one part's arrays. A program takes and returns all parts, laid end to end along the dimension named above; an argument that names none is the same for every part. Nothing has to cross between parts.
Inputs may be any that keep to these rules, and one draw needn't show every extreme that they name: `group_choice`: in each aligned block of 64 tokens every group is chosen by exactly 32 tokens. `member_choice`: each row names 2 different experts of its token's group. In each aligned block of 64 rows no expert (group and member together) is named by more than 32 rows, some expert is named by exactly 32 rows, and one expert is named by exactly 32 rows in every block.
All inputs are finite; a program needn't handle non-finite values.
Results may differ from the reference program's by a relative error of at most 0.017.
Values may be sent and summed in bfloat16 or wider, within the bound.
A program may use at most 64 MiB of HBM per device.

```python
import jax
import jax.numpy as jnp
from jax import lax

D = 4096
FF = 1024
TOK_DEV = 64
EXPERTS = 4
GROUPS = 2
PER_GROUP = 2
TOP = 2
CAP = 32
TOKENS = 256
N_EP = 4
N_TP = 4


def block_order(block_key):
    return jax.random.permutation(block_key, TOK_DEV)


def routing_draw(key):
    order_keys = jax.random.split(jax.random.fold_in(key, 101), N_EP)
    orderings = jax.vmap(block_order)(order_keys).astype(jnp.int32)
    groups_of = (orderings // CAP).astype(jnp.int32)
    favourite = jax.random.randint(jax.random.fold_in(key, 102), (GROUPS,), 0, PER_GROUP)
    coin_flip = jax.random.randint(jax.random.fold_in(key, 103), (N_EP, GROUPS), 0, 2)
    others = jax.random.randint(jax.random.fold_in(key, 104), (N_EP, GROUPS), 0, PER_GROUP)
    hot_member = jnp.where(coin_flip == 1, favourite[None, :], others)
    hot_member = hot_member.at[:, 0].set(favourite[0])
    token_hot = jnp.take_along_axis(hot_member, groups_of, axis=1)
    member_iota = jnp.arange(PER_GROUP, dtype=jnp.int32)
    raw_scores = jax.random.randint(jax.random.fold_in(key, 105), (N_EP, TOK_DEV, PER_GROUP), 0, 1 << 20)
    ranking = raw_scores * PER_GROUP + member_iota[None, None, :]
    ranking = jnp.where(member_iota[None, None, :] == token_hot[:, :, None], -1, ranking)
    members = jnp.argsort(ranking, axis=2)[:, :, :TOP]
    shuffle_scores = jax.random.randint(jax.random.fold_in(key, 106), (N_EP, TOK_DEV, TOP), 0, 1 << 20)
    shuffle_scores = shuffle_scores * TOP + jnp.arange(TOP, dtype=jnp.int32)[None, None, :]
    members = jnp.take_along_axis(members, jnp.argsort(shuffle_scores, axis=2), axis=2)
    return (groups_of.reshape(TOKENS).astype(jnp.int32), members.reshape(TOKENS, TOP).astype(jnp.int32))


def draw_group_choice(key, part):
    return routing_draw(key)[0]


def draw_member_choice(key, part):
    return routing_draw(key)[1]


def draw_tokens(key, part):
    col_pos = jnp.arange(D, dtype=jnp.float32) / D
    col_jitter = jax.random.uniform(jax.random.fold_in(key, 201), (D,), jnp.float32)
    col_scale = jnp.exp(jnp.log(10.0) * (0.5 * col_pos + 0.5 * col_jitter))
    row_scale = jnp.exp(jax.random.uniform(jax.random.fold_in(key, 202), (TOKENS, 1), jnp.float32, minval=jnp.log(0.3), maxval=jnp.log(3.0)))
    base = jnp.clip(jax.random.normal(jax.random.fold_in(key, 203), (TOKENS, D), jnp.float32), -6.0, 6.0)
    return (0.15 * base * row_scale * col_scale[None, :]).astype(jnp.bfloat16)


def block_scale(key, extent, cuts, low, top_value):
    gain, own = 1.0, jax.random.fold_in(key, 6)
    for dim, parts in cuts:
        heights = jnp.exp(jax.random.uniform(jax.random.fold_in(own, dim), (parts,), jnp.float32, low / len(cuts), top_value / len(cuts)))
        gain = gain * jnp.repeat(heights, extent[dim] // parts).reshape([-1 if axis == dim else 1 for axis in range(len(extent))])
    return gain


def normal_values(stream_key, extent, spread, reach, cuts=(), kind=jnp.bfloat16):
    values = jax.random.normal(stream_key, extent, jnp.float32) * spread
    if len(cuts) > 0:
        values = block_scale(stream_key, extent, cuts, -0.22, 0.18) * values
    return jnp.clip(values, min=-reach, max=reach).astype(kind)


def setup_inputs(seed: int = 0, part: int = 0) -> dict:
    streams_of = jax.random.split(jax.random.key(seed), 11)
    part_keys = jax.random.split(jax.random.fold_in(streams_of[10], part), 11)
    return {
        "tokens": draw_tokens(jax.random.fold_in(jax.random.fold_in(streams_of[10], part), 71), part),
        "group_choice": draw_group_choice(jax.random.fold_in(jax.random.fold_in(streams_of[10], part), 71), part),
        "member_choice": draw_member_choice(jax.random.fold_in(jax.random.fold_in(streams_of[10], part), 71), part),
        "group_prob": jnp.clip(0.3 + 0.7 * jax.random.uniform(part_keys[3], (TOKENS,), jnp.float32) ** block_scale(part_keys[3], (TOKENS,), ((0, 4),), -0.2, 0.2), 0.3, 1.0),
        "member_score": normal_values(part_keys[4], (TOKENS, TOP), 1.5, 4.0, ((0, 4),), jnp.float32),
        "norm_gain": jnp.clip(1.0 + 0.18 * jax.random.normal(streams_of[5], (D,), jnp.float32), 0.1, 1.9),
        "w_gate": normal_values(streams_of[6], (EXPERTS, D, FF), D ** -0.5, 0.09375, ((0, 4), (1, 4))),
        "w_up": normal_values(streams_of[7], (EXPERTS, D, FF), D ** -0.5, 0.09375, ((0, 4), (1, 4))),
        "w_down": normal_values(streams_of[8], (EXPERTS, FF, D), FF ** -0.5, 0.1875, ((0, 4), (2, 4))),
        "final_gain": jnp.clip(1.0 + 0.18 * jax.random.normal(streams_of[9], (D,), jnp.float32), 0.1, 1.9),
    }


EPS = 1e-06

def reference(tokens, group_choice, member_choice, group_prob, member_score, norm_gain, w_gate, w_up, w_down, final_gain):
    values = tokens.astype(jnp.float32)
    square_in = lax.optimization_barrier(jnp.sum(values * values, axis=1, keepdims=True))
    normed = (values * lax.rsqrt(square_in / D + EPS) * norm_gain.astype(jnp.float32)).astype(jnp.bfloat16)
    expert_ids = (group_choice[:, None] * PER_GROUP + member_choice).astype(jnp.int32)
    scores = jnp.exp(member_score)
    weights = group_prob[:, None] * scores / lax.optimization_barrier(jnp.sum(scores, axis=1, keepdims=True))
    blocks = normed.reshape(N_EP, TOK_DEV, D).astype(jnp.float32)
    slot_iota = jnp.arange(CAP, dtype=jnp.int32)

    def one_expert(carried, expert):
        chosen = expert_ids == expert
        counted = lax.optimization_barrier(jnp.sum(chosen.astype(jnp.int32), axis=1)).reshape(N_EP, TOK_DEV)
        weight_mine = lax.optimization_barrier(jnp.sum(jnp.where(chosen, weights, jnp.float32(0.0)), axis=1)).reshape(TOKENS, 1)
        position = jnp.cumsum(counted, axis=1) - counted
        slot_pick = ((position[:, None, :] == slot_iota[None, :, None]) & (counted[:, None, :] > 0)).astype(jnp.float32)
        rows_in = jnp.einsum('sct,std->scd', slot_pick, blocks).astype(jnp.bfloat16)
        rows_in = rows_in.reshape(N_EP * CAP, N_TP, D // N_TP).astype(jnp.float32)
        gate_w = lax.dynamic_index_in_dim(w_gate, expert, 0, keepdims=False).reshape(N_TP, D // N_TP, FF)
        up_w = lax.dynamic_index_in_dim(w_up, expert, 0, keepdims=False).reshape(N_TP, D // N_TP, FF)
        down_w = lax.dynamic_index_in_dim(w_down, expert, 0, keepdims=False)
        gate_part = jnp.einsum('rpd,pdf->prf', rows_in, gate_w.astype(jnp.float32)).astype(jnp.bfloat16)
        up_part = jnp.einsum('rpd,pdf->prf', rows_in, up_w.astype(jnp.float32)).astype(jnp.bfloat16)
        gate_part, up_part = lax.optimization_barrier((gate_part, up_part))
        gate_sum = lax.optimization_barrier(jnp.sum(gate_part.astype(jnp.float32), axis=0))
        up_sum = lax.optimization_barrier(jnp.sum(up_part.astype(jnp.float32), axis=0))
        hidden = (jax.nn.silu(gate_sum) * up_sum).astype(jnp.bfloat16)
        rows_out = jnp.dot(hidden, down_w, preferred_element_type=jnp.float32).astype(jnp.bfloat16)
        rows_out = rows_out.reshape(N_EP, CAP, D).astype(jnp.float32)
        returned = jnp.einsum('sct,scd->std', slot_pick, rows_out).reshape(TOKENS, D)
        return (carried + returned * weight_mine, expert)
    moe, unused = lax.scan(one_expert, jnp.zeros((TOKENS, D), jnp.float32), jnp.arange(EXPERTS, dtype=jnp.int32))
    summed = values + moe
    square_out = lax.optimization_barrier(jnp.sum(summed * summed, axis=1, keepdims=True))
    return (summed * lax.rsqrt(square_out / D + EPS) * final_gain.astype(jnp.float32)).astype(jnp.bfloat16)
```

```python
import functools

import jax
import jax.numpy as jnp
from jax import lax
from jax.experimental import pallas as pl
from jax.experimental.pallas import tpu as pltpu
from jax.sharding import PartitionSpec as P

EPS = 1e-06
MESH = pl.DeviceIdType.MESH
F32 = jnp.float32
BF16 = jnp.bfloat16


def partner(me, s, n):
    out, bit = me, 1
    while bit < n:
        if s & bit:
            out = out + bit - 2 * bit * ((me // bit) % 2)
        bit *= 2
    return out


def iota(shape, dim):
    return lax.broadcasted_iota(jnp.int32, shape, dim)


def to_row(col, width):
    n = col.shape[0]
    eye = iota((n, width), 0) == iota((n, width), 1)
    return jnp.sum(jnp.where(eye, col, 0.0), axis=0, keepdims=True)


def to_col(row, n):
    width = row.shape[1]
    eye = iota((n, width), 0) == iota((n, width), 1)
    return jnp.sum(jnp.where(eye, row, 0.0), axis=1, keepdims=True)


def kernel(
    cfg,
    x_ref,
    group_ref,
    member_ref,
    prob_ref,
    score_ref,
    ngain_ref,
    wg_hbm,
    wu_hbm,
    wd_hbm,
    fgain_ref,
    out_ref,
    wg,
    wu,
    wd,
    xs,
    xr,
    ps,
    pr,
    sqs,
    sqr,
    hs,
    hr,
    ob,
    ret,
    fs,
    fr,
    w_sem,
    x_send,
    x_recv,
    p_send,
    p_recv,
    q_send,
    q_recv,
    h_send,
    h_recv,
    o_send,
    o_recv,
    f_send,
    f_recv,
):
    n_ep, n_tp, groups, chunks = cfg
    per_group = n_ep // groups
    tok, dim = x_ref.shape
    cap = tok // groups
    ff = wg.shape[1]
    q = ff // n_tp
    full_width = dim * n_tp
    me_e = lax.axis_index("ep")
    me_t = lax.axis_index("tp")

    barrier = pltpu.get_barrier_semaphore()
    for s in range(1, n_ep):
        pl.semaphore_signal(barrier, inc=1, device_id={"ep": partner(me_e, s, n_ep)}, device_id_type=MESH)
    for s in range(1, n_tp):
        pl.semaphore_signal(barrier, inc=1, device_id={"tp": partner(me_t, s, n_tp)}, device_id_type=MESH)

    loads = [
        pltpu.make_async_copy(src.at[0], dst, w_sem.at[i])
        for i, (src, dst) in enumerate(((wg_hbm, wg), (wu_hbm, wu), (wd_hbm, wd)))
    ]
    for load in loads:
        load.start()

    group_row = group_ref[...]
    rows8 = max(8, groups)
    onehot = (iota((rows8, tok), 0) == group_row).astype(F32)
    strict = (iota((tok, tok), 0) < iota((tok, tok), 1)).astype(F32)
    rank = jnp.dot(onehot.astype(BF16), strict.astype(BF16), preferred_element_type=F32)
    slot_row = jnp.sum(
        onehot * (iota((rows8, tok), 0).astype(F32) * cap + rank), axis=0, keepdims=True
    )
    picker = (iota((tok, tok), 0).astype(F32) == slot_row).astype(BF16)
    x = x_ref[...]
    xs[...] = jnp.dot(picker, x, preferred_element_type=F32).astype(BF16)

    pl.semaphore_wait(barrier, n_ep - 1 + n_tp - 1)

    pending = []

    def send(src, dst, ssem, rsem, where):
        copy = pltpu.make_async_remote_copy(
            src_ref=src, dst_ref=dst, send_sem=ssem, recv_sem=rsem, device_id=where, device_id_type=MESH
        )
        copy.start()
        pending.append(copy)
        return copy

    def group_rows(e):
        return pl.ds(pl.multiple_of((e // per_group) * cap, cap), cap)

    x_copies = {}
    for s in range(1, n_ep):
        e = partner(me_e, s, n_ep)
        x_copies[s] = send(
            xs.at[group_rows(e)], xr.at[pl.ds(s * cap, cap)], x_send.at[s], x_recv.at[s], {"ep": e}
        )
    xr[pl.ds(0, cap), :] = xs[group_rows(me_e), :]

    ngain = ngain_ref[...]
    tp_order = [s for s in range(2, n_tp)] + [s for s in range(1, min(2, n_tp))]
    p_copies, q_copies, h_copies, o_copies = {}, {}, {}, {}
    own_parts, own_sq = {}, {}

    def span(c):
        first, count = chunks[c]
        return first * cap, count * cap

    def stage_a(c):
        first, count = chunks[c]
        start, rows = span(c)
        for s in range(first, first + count):
            if s > 0:
                x_copies[s].wait_recv()
        vals = xr[pl.ds(start, rows), :].astype(F32)
        sq = jnp.sum(vals * vals, axis=1, keepdims=True)
        own_sq[c] = sq
        width = sqs.shape[2]
        sqs[c] = jnp.broadcast_to(to_row(sq, width), (8, width))
        for s in tp_order:
            q_copies[c, s] = send(
                sqs.at[c], sqr.at[c, s], q_send.at[c, s], q_recv.at[c, s], {"tp": partner(me_t, s, n_tp)}
            )
        rows_in = (vals * ngain).astype(BF16)
        if c == 0:
            loads[0].wait()
            loads[1].wait()
        for s in tp_order + [0]:
            p = partner(me_t, s, n_tp)
            cols = pl.ds(pl.multiple_of(p * q, q), q)
            g = jnp.dot(rows_in, wg[:, cols], preferred_element_type=F32).astype(BF16)
            u = jnp.dot(rows_in, wu[:, cols], preferred_element_type=F32).astype(BF16)
            if s == 0:
                own_parts[c] = (g, u)
            else:
                ps[s, pl.ds(start, rows), pl.ds(0, q)] = g
                ps[s, pl.ds(start, rows), pl.ds(q, q)] = u
                p_copies[c, s] = send(
                    ps.at[s, pl.ds(start, rows)],
                    pr.at[s, pl.ds(start, rows)],
                    p_send.at[c, s],
                    p_recv.at[c, s],
                    {"tp": p},
                )

    def stage_b(c):
        start, rows = span(c)
        total = own_sq[c]
        for s in range(1, n_tp):
            q_copies[c, s].wait_recv()
            total = total + to_col(sqr[c, s][0:1, :], rows)
        scale = lax.rsqrt(total / full_width + EPS)
        g, u = own_parts[c]
        g, u = g.astype(F32), u.astype(F32)
        for s in range(1, n_tp):
            p_copies[c, s].wait_recv()
            g = g + pr[s, pl.ds(start, rows), pl.ds(0, q)].astype(F32)
            u = u + pr[s, pl.ds(start, rows), pl.ds(q, q)].astype(F32)
        g, u = g * scale, u * scale
        hidden = (g / (1.0 + jnp.exp(-g)) * u).astype(BF16)
        hs[pl.ds(start, rows), :] = hidden
        for s in tp_order:
            h_copies[c, s] = send(
                hs.at[pl.ds(start, rows)],
                hr.at[s, pl.ds(start, rows)],
                h_send.at[c, s],
                h_recv.at[c, s],
                {"tp": partner(me_t, s, n_tp)},
            )

    def stage_c(c):
        first, count = chunks[c]
        start, rows = span(c)
        if c == 0:
            loads[2].wait()
        acc = None
        for s in range(n_tp):
            if s > 0:
                h_copies[c, s].wait_recv()
                h = hr[s, pl.ds(start, rows), :]
            else:
                h = hs[pl.ds(start, rows), :]
            p = partner(me_t, s, n_tp)
            term = jnp.dot(h, wd[pl.ds(pl.multiple_of(p * q, q), q), :], preferred_element_type=F32)
            acc = term if acc is None else acc + term
        ob[pl.ds(start, rows), :] = acc.astype(BF16)
        for s in range(first, first + count):
            if s > 0:
                o_copies[s] = send(
                    ob.at[pl.ds(s * cap, cap)],
                    ret.at[pl.ds(s * cap, cap)],
                    o_send.at[s],
                    o_recv.at[s],
                    {"ep": partner(me_e, s, n_ep)},
                )

    n_chunks = len(chunks)
    for step in range(n_chunks + 4):
        if step < n_chunks:
            stage_a(step)
        if 0 <= step - 1 < n_chunks:
            stage_b(step - 1)
        if 0 <= step - 2 < n_chunks:
            stage_c(step - 2)

    scores = jnp.exp(score_ref[...])
    weights = to_col(prob_ref[...], tok) * scores / jnp.sum(scores, axis=1, keepdims=True)
    slot_col = to_col(slot_row, tok).astype(jnp.int32)
    ids = to_col(group_row.astype(F32), tok).astype(jnp.int32) * per_group + member_ref[...]
    summed = x.astype(F32)
    for s in range(n_ep):
        e = partner(me_e, s, n_ep)
        if s > 0:
            o_copies[s].wait_recv()
            rows = ret[pl.ds(s * cap, cap), :]
        else:
            rows = ob[pl.ds(0, cap), :]
        pick = (iota((tok, cap), 1) + (e // per_group) * cap == slot_col).astype(F32).astype(BF16)
        weight = jnp.sum(jnp.where(ids == e, weights, 0.0), axis=1, keepdims=True)
        summed = summed + weight * jnp.dot(pick, rows, preferred_element_type=F32)

    square = jnp.sum(summed * summed, axis=1, keepdims=True)
    width = fs.shape[1]
    fs[...] = jnp.broadcast_to(to_row(square, width), (8, width))
    f_copies = {}
    for s in tp_order:
        f_copies[s] = send(fs, fr.at[s], f_send.at[s], f_recv.at[s], {"tp": partner(me_t, s, n_tp)})
    for s in range(1, n_tp):
        f_copies[s].wait_recv()
        square = square + to_col(fr[s][0:1, :], tok)
    out_ref[...] = (summed * lax.rsqrt(square / full_width + EPS) * fgain_ref[...]).astype(BF16)

    for copy in pending:
        copy.wait_send()


def solution(mesh):
    n_ep, n_tp = mesh.shape["ep"], mesh.shape["tp"]
    groups = max(2, n_ep // 8)
    n_chunks = 4
    each = n_ep // n_chunks
    chunks = tuple((i * each, each) for i in range(n_chunks))

    def local(tokens, group_choice, member_choice, group_prob, member_score, norm_gain, w_gate, w_up, w_down, final_gain):
        tok, dim = tokens.shape
        ff = w_gate.shape[2]
        cap = tok // groups
        q = ff // n_tp
        all_rows = n_ep * cap
        width = -(-max(count * cap for _, count in chunks) // 128) * 128
        out_width = -(-tok // 128) * 128
        vmem = pl.BlockSpec(memory_space=pltpu.VMEM)
        hbm = pl.BlockSpec(memory_space=pl.ANY)
        dma = pltpu.SemaphoreType.DMA
        nc = len(chunks)
        return pl.pallas_call(
            functools.partial(kernel, (n_ep, n_tp, groups, chunks)),
            out_shape=jax.ShapeDtypeStruct((tok, dim), BF16),
            in_specs=[vmem] * 6 + [hbm] * 3 + [vmem],
            out_specs=vmem,
            scratch_shapes=[
                pltpu.VMEM((dim, ff), BF16),
                pltpu.VMEM((dim, ff), BF16),
                pltpu.VMEM((ff, dim), BF16),
                pltpu.VMEM((tok, dim), BF16),
                pltpu.VMEM((all_rows, dim), BF16),
                pltpu.VMEM((n_tp, all_rows, 2 * q), BF16),
                pltpu.VMEM((n_tp, all_rows, 2 * q), BF16),
                pltpu.VMEM((nc, 8, width), F32),
                pltpu.VMEM((nc, n_tp, 8, width), F32),
                pltpu.VMEM((all_rows, q), BF16),
                pltpu.VMEM((n_tp, all_rows, q), BF16),
                pltpu.VMEM((all_rows, dim), BF16),
                pltpu.VMEM((all_rows, dim), BF16),
                pltpu.VMEM((8, out_width), F32),
                pltpu.VMEM((n_tp, 8, out_width), F32),
                dma((3,)),
                dma((n_ep,)),
                dma((n_ep,)),
                dma((nc, n_tp)),
                dma((nc, n_tp)),
                dma((nc, n_tp)),
                dma((nc, n_tp)),
                dma((nc, n_tp)),
                dma((nc, n_tp)),
                dma((n_ep,)),
                dma((n_ep,)),
                dma((n_tp,)),
                dma((n_tp,)),
            ],
            compiler_params=pltpu.CompilerParams(collective_id=0, has_side_effects=True),
        )(
            tokens,
            group_choice.reshape(1, tok),
            member_choice,
            group_prob.reshape(1, tok),
            member_score,
            norm_gain.reshape(1, dim),
            w_gate,
            w_up,
            w_down,
            final_gain.reshape(1, dim),
        )

    return jax.shard_map(
        local,
        mesh=mesh,
        in_specs=(
            P(("grp", "ep"), "tp"),
            P(("grp", "ep")),
            P(("grp", "ep"), None),
            P(("grp", "ep")),
            P(("grp", "ep"), None),
            P("tp"),
            P("ep", "tp", None),
            P("ep", "tp", None),
            P("ep", None, "tp"),
            P("tp"),
        ),
        out_specs=P(("grp", "ep"), "tp"),
        check_vma=False,
    )
```

```python
import functools

import jax
import jax.numpy as jnp
from jax import lax
from jax.experimental import pallas as pl
from jax.experimental.pallas import tpu as pltpu
from jax.sharding import PartitionSpec as P

EPS = 1e-06
MESH = pl.DeviceIdType.MESH
F32 = jnp.float32
BF16 = jnp.bfloat16
PLAN = (
    ("a", 0), ("a", 1), ("b", 0), ("a", 2), ("a", 3), ("b", 1),
    ("c", 0), ("b", 2), ("b", 3), ("c", 1), ("c", 2), ("c", 3),
)
VMEM_LIMIT = 60 * 2**20


def partner(me, s, n):
    out, bit = me, 1
    while bit < n:
        if s & bit:
            out = out + bit - 2 * bit * ((me // bit) % 2)
        bit *= 2
    return out


def iota(shape, dim):
    return lax.broadcasted_iota(jnp.int32, shape, dim)


def to_row(col, width):
    n = col.shape[0]
    eye = iota((n, width), 0) == iota((n, width), 1)
    return jnp.sum(jnp.where(eye, col, 0.0), axis=0, keepdims=True)


def to_col(row, n):
    width = row.shape[1]
    eye = iota((n, width), 0) == iota((n, width), 1)
    return jnp.sum(jnp.where(eye, row, 0.0), axis=1, keepdims=True)


def kernel(
    cfg,
    x_hbm,
    group_hbm,
    member_hbm,
    prob_hbm,
    score_hbm,
    ngain_hbm,
    wg_hbm,
    wu_hbm,
    wd_hbm,
    out_ref,
    x_ref,
    group_ref,
    member_ref,
    prob_ref,
    score_ref,
    ngain_ref,
    wg,
    wu,
    wd,
    xs,
    xr,
    ps,
    pr,
    sqs,
    sqr,
    hs,
    hr,
    ob,
    ret,
    fs,
    fr,
    w_sem,
    x_send,
    x_recv,
    p_send,
    p_recv,
    q_send,
    q_recv,
    h_send,
    h_recv,
    o_send,
    o_recv,
    f_send,
    f_recv,
):
    n_ep, n_tp, groups, order, chunks = cfg
    per_group = n_ep // groups
    tok, dim = x_ref.shape
    cap = tok // groups
    ff = wg.shape[1]
    q = ff // n_tp
    full_width = dim * n_tp
    me_e = lax.axis_index("ep")
    me_t = lax.axis_index("tp")

    barrier = pltpu.get_barrier_semaphore()
    for s in range(1, n_ep):
        pl.semaphore_signal(barrier, inc=1, device_id={"ep": partner(me_e, s, n_ep)}, device_id_type=MESH)
    for s in range(1, n_tp):
        pl.semaphore_signal(barrier, inc=1, device_id={"tp": partner(me_t, s, n_tp)}, device_id_type=MESH)

    moves = (
        (group_hbm, group_ref),
        (x_hbm, x_ref),
        (ngain_hbm, ngain_ref),
        (wg_hbm.at[0], wg),
        (wu_hbm.at[0], wu),
        (member_hbm, member_ref),
        (prob_hbm, prob_ref),
        (score_hbm, score_ref),
        (wd_hbm.at[0], wd),
    )
    loads = [pltpu.make_async_copy(src, dst, w_sem.at[i]) for i, (src, dst) in enumerate(moves)]
    for load in loads:
        load.start()
    loads[0].wait()
    loads[1].wait()

    group_row = group_ref[...]
    rows8 = max(8, groups)
    onehot = (iota((rows8, tok), 0) == group_row).astype(F32)
    strict = (iota((tok, tok), 0) < iota((tok, tok), 1)).astype(F32)
    rank = jnp.dot(onehot.astype(BF16), strict.astype(BF16), preferred_element_type=F32)
    slot_row = jnp.sum(
        onehot * (iota((rows8, tok), 0).astype(F32) * cap + rank), axis=0, keepdims=True
    )
    picker = (iota((tok, tok), 0).astype(F32) == slot_row).astype(BF16)
    x = x_ref[...]
    xs[...] = jnp.dot(picker, x, preferred_element_type=F32).astype(BF16)

    pending = []

    def send(src, dst, ssem, rsem, where):
        copy = pltpu.make_async_remote_copy(
            src_ref=src, dst_ref=dst, send_sem=ssem, recv_sem=rsem, device_id=where, device_id_type=MESH
        )
        copy.start()
        pending.append(copy)
        return copy

    def group_rows(e):
        return pl.ds(pl.multiple_of((e // per_group) * cap, cap), cap)

    xr[pl.ds(0, cap), :] = xs[group_rows(me_e), :]
    x_copies = {}

    def dispatch():
        for k in range(1, n_ep):
            e = partner(me_e, order[k], n_ep)
            x_copies[k] = send(
                xs.at[group_rows(e)], xr.at[pl.ds(k * cap, cap)], x_send.at[k], x_recv.at[k], {"ep": e}
            )

    loads[2].wait()
    ngain = ngain_ref[...]
    tp_order = [s for s in range(2, n_tp)] + [s for s in range(1, min(2, n_tp))]
    p_copies, q_copies, h_copies, o_copies = {}, {}, {}, {}
    own_sq = {}

    def span(c):
        first, count = chunks[c]
        return first * cap, count * cap

    def products(c):
        start, rows = span(c)
        vals = xr[pl.ds(start, rows), :].astype(F32)
        sq = jnp.sum(vals * vals, axis=1, keepdims=True)
        own_sq[c] = sq
        width = sqs.shape[2]
        sqs[c] = jnp.broadcast_to(to_row(sq, width), (8, width))
        rows_in = (vals * ngain).astype(BF16)
        for s in tp_order + [0]:
            p = partner(me_t, s, n_tp)
            cols = pl.ds(pl.multiple_of(p * q, q), q)
            ps[s, pl.ds(start, rows), pl.ds(0, q)] = jnp.dot(
                rows_in, wg[:, cols], preferred_element_type=F32
            ).astype(BF16)
            ps[s, pl.ds(start, rows), pl.ds(q, q)] = jnp.dot(
                rows_in, wu[:, cols], preferred_element_type=F32
            ).astype(BF16)
            if s > 0:
                send_part(c, s)

    def send_part(c, s):
        start, rows = span(c)
        peer = {"tp": partner(me_t, s, n_tp)}
        p_copies[c, s] = send(
            ps.at[s, pl.ds(start, rows)],
            pr.at[s, pl.ds(start, rows)],
            p_send.at[c, s],
            p_recv.at[c, s],
            peer,
        )
        q_copies[c, s] = send(sqs.at[c], sqr.at[c, s], q_send.at[c, s], q_recv.at[c, s], peer)

    def stage_a(c):
        first, count = chunks[c]
        for k in range(max(first, 1), first + count):
            x_copies[k].wait_recv()
        products(c)

    def stage_b(c):
        start, rows = span(c)
        total = own_sq[c]
        for s in range(1, n_tp):
            q_copies[c, s].wait_recv()
            total = total + to_col(sqr[c, s][0:1, :], rows)
        scale = lax.rsqrt(total / full_width + EPS)
        g = ps[0, pl.ds(start, rows), pl.ds(0, q)].astype(F32)
        u = ps[0, pl.ds(start, rows), pl.ds(q, q)].astype(F32)
        for s in range(1, n_tp):
            p_copies[c, s].wait_recv()
            g = g + pr[s, pl.ds(start, rows), pl.ds(0, q)].astype(F32)
            u = u + pr[s, pl.ds(start, rows), pl.ds(q, q)].astype(F32)
        g, u = g * scale, u * scale
        hidden = (g / (1.0 + jnp.exp(-g)) * u).astype(BF16)
        hs[pl.ds(start, rows), :] = hidden
        for s in tp_order:
            h_copies[c, s] = send(
                hs.at[pl.ds(start, rows)],
                hr.at[s, pl.ds(start, rows)],
                h_send.at[c, s],
                h_recv.at[c, s],
                {"tp": partner(me_t, s, n_tp)},
            )

    def stage_c(c):
        first, count = chunks[c]
        start, rows = span(c)
        if c == 0:
            loads[8].wait()
        acc = None
        for s in range(n_tp):
            if s > 0:
                h_copies[c, s].wait_recv()
                h = hr[s, pl.ds(start, rows), :]
            else:
                h = hs[pl.ds(start, rows), :]
            p = partner(me_t, s, n_tp)
            term = jnp.dot(h, wd[pl.ds(pl.multiple_of(p * q, q), q), :], preferred_element_type=F32)
            acc = term if acc is None else acc + term
        ob[pl.ds(start, rows), :] = acc.astype(BF16)
        for k in range(first, first + count):
            if k > 0:
                o_copies[k] = send(
                    ob.at[pl.ds(k * cap, cap)],
                    ret.at[pl.ds(k * cap, cap)],
                    o_send.at[k],
                    o_recv.at[k],
                    {"ep": partner(me_e, order[k], n_ep)},
                )

    pl.semaphore_wait(barrier, n_ep - 1 + n_tp - 1)
    dispatch()
    loads[3].wait()
    loads[4].wait()
    stage_a(0)
    for load in loads[5:8]:
        load.wait()
    scores = jnp.exp(score_ref[...])
    weights = prob_ref[...] * scores / jnp.sum(scores, axis=0, keepdims=True)
    slot_col = to_col(slot_row, tok).astype(jnp.int32)
    ids = group_row * per_group + member_ref[...]
    expert_cols = []
    for k in range(n_ep):
        named = jnp.where(ids == partner(me_e, order[k], n_ep), weights, 0.0)
        expert_cols.append(to_col(jnp.sum(named, axis=0, keepdims=True), tok))

    stages = {"a": stage_a, "b": stage_b, "c": stage_c}
    for stage, c in PLAN[1:]:
        stages[stage](c)

    summed = x.astype(F32)
    for k in range(n_ep):
        e = partner(me_e, order[k], n_ep)
        if k > 0:
            o_copies[k].wait_recv()
            rows = ret[pl.ds(k * cap, cap), :]
        else:
            rows = ob[pl.ds(0, cap), :]
        pick = (iota((tok, cap), 1) + (e // per_group) * cap == slot_col).astype(F32).astype(BF16)
        summed = summed + expert_cols[k] * jnp.dot(pick, rows, preferred_element_type=F32)

    square = jnp.sum(summed * summed, axis=1, keepdims=True)
    width = fs.shape[1]
    fs[...] = jnp.broadcast_to(to_row(square, width), (8, width))
    f_copies = {}
    for s in tp_order:
        f_copies[s] = send(fs, fr.at[s], f_send.at[s], f_recv.at[s], {"tp": partner(me_t, s, n_tp)})
    for s in range(1, n_tp):
        f_copies[s].wait_recv()
        square = square + to_col(fr[s][0:1, :], tok)
    out_ref[...] = summed * lax.rsqrt(square / full_width + EPS)

    for copy in pending:
        copy.wait_send()


def solution(mesh):
    n_ep, n_tp = mesh.shape["ep"], mesh.shape["tp"]
    groups = max(2, n_ep // 8)
    order = range(n_ep)
    n_chunks = 4
    each = n_ep // n_chunks
    chunks = tuple((i * each, each) for i in range(n_chunks))

    def local(tokens, group_choice, member_choice, group_prob, member_score, norm_gain, w_gate, w_up, w_down, final_gain):
        tok, dim = tokens.shape
        ff, top = w_gate.shape[2], member_choice.shape[1]
        cap = tok // groups
        q = ff // n_tp
        all_rows = n_ep * cap
        width = -(-max(count * cap for _, count in chunks) // 128) * 128
        out_width = -(-tok // 128) * 128
        vmem = pl.BlockSpec(memory_space=pltpu.VMEM)
        hbm = pl.BlockSpec(memory_space=pltpu.HBM)
        dma = pltpu.SemaphoreType.DMA
        nc = len(chunks)
        normal = pl.pallas_call(
            functools.partial(kernel, (n_ep, n_tp, groups, tuple(order), chunks)),
            out_shape=jax.ShapeDtypeStruct((tok, dim), F32),
            in_specs=[hbm] * 9,
            out_specs=vmem,
            scratch_shapes=[
                pltpu.VMEM((tok, dim), BF16),
                pltpu.VMEM((1, tok), jnp.int32),
                pltpu.VMEM((top, tok), jnp.int32),
                pltpu.VMEM((1, tok), F32),
                pltpu.VMEM((top, tok), F32),
                pltpu.VMEM((1, dim), F32),
                pltpu.VMEM((dim, ff), BF16),
                pltpu.VMEM((dim, ff), BF16),
                pltpu.VMEM((ff, dim), BF16),
                pltpu.VMEM((tok, dim), BF16),
                pltpu.VMEM((all_rows, dim), BF16),
                pltpu.VMEM((n_tp, all_rows, 2 * q), BF16),
                pltpu.VMEM((n_tp, all_rows, 2 * q), BF16),
                pltpu.VMEM((nc, 8, width), F32),
                pltpu.VMEM((nc, n_tp, 8, width), F32),
                pltpu.VMEM((all_rows, q), BF16),
                pltpu.VMEM((n_tp, all_rows, q), BF16),
                pltpu.VMEM((all_rows, dim), BF16),
                pltpu.VMEM((all_rows, dim), BF16),
                pltpu.VMEM((8, out_width), F32),
                pltpu.VMEM((n_tp, 8, out_width), F32),
                dma((9,)),
                dma((n_ep,)),
                dma((n_ep,)),
                dma((nc, n_tp)),
                dma((nc, n_tp)),
                dma((nc, n_tp)),
                dma((nc, n_tp)),
                dma((nc, n_tp)),
                dma((nc, n_tp)),
                dma((n_ep,)),
                dma((n_ep,)),
                dma((n_tp,)),
                dma((n_tp,)),
            ],
            compiler_params=pltpu.CompilerParams(collective_id=0, has_side_effects=True, vmem_limit_bytes=VMEM_LIMIT),
        )(
            tokens,
            group_choice.reshape(1, tok),
            member_choice.T,
            group_prob.reshape(1, tok),
            member_score.T,
            norm_gain.reshape(1, dim),
            w_gate,
            w_up,
            w_down,
        )
        return (normal * final_gain[None, :]).astype(BF16)

    return jax.shard_map(
        local,
        mesh=mesh,
        in_specs=(
            P(("grp", "ep"), "tp"),
            P(("grp", "ep")),
            P(("grp", "ep"), None),
            P(("grp", "ep")),
            P(("grp", "ep"), None),
            P("tp"),
            P("ep", "tp", None),
            P("ep", "tp", None),
            P("ep", None, "tp"),
            P("tp"),
        ),
        out_specs=P(("grp", "ep"), "tp"),
        check_vma=False,
    )
```

```python
import functools

import jax
import jax.numpy as jnp
from jax import lax
from jax.experimental import pallas as pl
from jax.experimental.pallas import tpu as pltpu
from jax.sharding import PartitionSpec as P

EPS = 1e-06
MESH = pl.DeviceIdType.MESH
F32 = jnp.float32
BF16 = jnp.bfloat16
PLAN = (
    ("a", 0), ("a", 1), ("b", 0), ("a", 2), ("a", 3), ("b", 1),
    ("c", 0), ("b", 2), ("b", 3), ("c", 2), ("c", 1), ("c", 3),
)
VMEM_LIMIT = 56 * 2**20


def partner(me, s, n):
    out, bit = me, 1
    while bit < n:
        if s & bit:
            out = out + bit - 2 * bit * ((me // bit) % 2)
        bit *= 2
    return out


def iota(shape, dim):
    return lax.broadcasted_iota(jnp.int32, shape, dim)


def to_row(col, width):
    n = col.shape[0]
    eye = iota((n, width), 0) == iota((n, width), 1)
    return jnp.sum(jnp.where(eye, col, 0.0), axis=0, keepdims=True)


def to_col(row, n):
    width = row.shape[1]
    eye = iota((n, width), 0) == iota((n, width), 1)
    return jnp.sum(jnp.where(eye, row, 0.0), axis=1, keepdims=True)


def kernel(
    cfg,
    x_hbm,
    group_hbm,
    member_hbm,
    prob_hbm,
    score_hbm,
    ngain_hbm,
    wg_hbm,
    wu_hbm,
    wd_hbm,
    out_ref,
    x_ref,
    group_ref,
    member_ref,
    prob_ref,
    score_ref,
    ngain_ref,
    wg,
    wu,
    wd,
    xs,
    xr,
    ps,
    pr,
    sqs,
    sqr,
    hs,
    hr,
    ob,
    ret,
    fs,
    fr,
    w_sem,
    x_send,
    x_recv,
    p_send,
    p_recv,
    q_send,
    q_recv,
    h_send,
    h_recv,
    o_send,
    o_recv,
    f_send,
    f_recv,
):
    n_ep, n_tp, groups, order, chunks = cfg
    per_group = n_ep // groups
    tok, dim = x_ref.shape
    cap = tok // groups
    ff = wg.shape[1]
    q = ff // n_tp
    full_width = dim * n_tp
    me_e = lax.axis_index("ep")
    me_t = lax.axis_index("tp")

    barrier = pltpu.get_barrier_semaphore()
    for s in range(1, n_ep):
        pl.semaphore_signal(barrier, inc=1, device_id={"ep": partner(me_e, s, n_ep)}, device_id_type=MESH)
    for s in range(1, n_tp):
        pl.semaphore_signal(barrier, inc=1, device_id={"tp": partner(me_t, s, n_tp)}, device_id_type=MESH)

    moves = (
        (group_hbm, group_ref),
        (x_hbm, x_ref),
        (ngain_hbm, ngain_ref),
        (wg_hbm.at[0], wg),
        (wu_hbm.at[0], wu),
        (member_hbm, member_ref),
        (prob_hbm, prob_ref),
        (score_hbm, score_ref),
        (wd_hbm.at[0], wd),
    )
    loads = [pltpu.make_async_copy(src, dst, w_sem.at[i]) for i, (src, dst) in enumerate(moves)]
    for load in loads:
        load.start()
    loads[0].wait()
    loads[1].wait()

    group_row = group_ref[...]
    rows8 = max(8, groups)
    onehot = (iota((rows8, tok), 0) == group_row).astype(F32)
    strict = (iota((tok, tok), 0) < iota((tok, tok), 1)).astype(F32)
    rank = jnp.dot(onehot.astype(BF16), strict.astype(BF16), preferred_element_type=F32)
    slot_row = jnp.sum(
        onehot * (iota((rows8, tok), 0).astype(F32) * cap + rank), axis=0, keepdims=True
    )
    picker = (iota((tok, tok), 0).astype(F32) == slot_row).astype(BF16)
    x = x_ref[...]
    xs[...] = jnp.dot(picker, x, preferred_element_type=F32).astype(BF16)

    pending = []

    def send(src, dst, ssem, rsem, where):
        copy = pltpu.make_async_remote_copy(
            src_ref=src, dst_ref=dst, send_sem=ssem, recv_sem=rsem, device_id=where, device_id_type=MESH
        )
        copy.start()
        pending.append(copy)
        return copy

    def group_rows(e):
        return pl.ds(pl.multiple_of((e // per_group) * cap, cap), cap)

    xr[pl.ds(0, cap), :] = xs[group_rows(me_e), :]
    x_copies = {}

    def dispatch():
        for k in range(1, n_ep):
            e = partner(me_e, order[k], n_ep)
            x_copies[k] = send(
                xs.at[group_rows(e)], xr.at[pl.ds(k * cap, cap)], x_send.at[k], x_recv.at[k], {"ep": e}
            )

    loads[2].wait()
    ngain = ngain_ref[...]
    tp_order = [s for s in range(2, n_tp)] + [s for s in range(1, min(2, n_tp))]
    p_copies, q_copies, h_copies, o_copies = {}, {}, {}, {}
    own_sq = {}

    def span(c):
        first, count = chunks[c]
        return first * cap, count * cap

    def products(c):
        start, rows = span(c)
        vals = xr[pl.ds(start, rows), :].astype(F32)
        sq = jnp.sum(vals * vals, axis=1, keepdims=True)
        own_sq[c] = sq
        width = sqs.shape[2]
        sqs[c] = jnp.broadcast_to(to_row(sq, width), (8, width))
        rows_in = (vals * ngain).astype(BF16)
        for s in tp_order + [0]:
            p = partner(me_t, s, n_tp)
            cols = pl.ds(pl.multiple_of(p * q, q), q)
            ps[s, pl.ds(start, rows), pl.ds(0, q)] = jnp.dot(
                rows_in, wg[:, cols], preferred_element_type=F32
            ).astype(BF16)
            ps[s, pl.ds(start, rows), pl.ds(q, q)] = jnp.dot(
                rows_in, wu[:, cols], preferred_element_type=F32
            ).astype(BF16)
            if s > 0:
                send_part(c, s)

    def send_part(c, s):
        start, rows = span(c)
        peer = {"tp": partner(me_t, s, n_tp)}
        p_copies[c, s] = send(
            ps.at[s, pl.ds(start, rows)],
            pr.at[s, pl.ds(start, rows)],
            p_send.at[c, s],
            p_recv.at[c, s],
            peer,
        )
        q_copies[c, s] = send(sqs.at[c], sqr.at[c, s], q_send.at[c, s], q_recv.at[c, s], peer)

    def stage_a(c):
        first, count = chunks[c]
        for k in range(max(first, 1), first + count):
            x_copies[k].wait_recv()
        products(c)

    def stage_b(c):
        start, rows = span(c)
        total = own_sq[c]
        for s in range(1, n_tp):
            q_copies[c, s].wait_recv()
            total = total + to_col(sqr[c, s][0:1, :], rows)
        scale = lax.rsqrt(total / full_width + EPS)
        g = ps[0, pl.ds(start, rows), pl.ds(0, q)].astype(F32)
        u = ps[0, pl.ds(start, rows), pl.ds(q, q)].astype(F32)
        for s in range(1, n_tp):
            p_copies[c, s].wait_recv()
            g = g + pr[s, pl.ds(start, rows), pl.ds(0, q)].astype(F32)
            u = u + pr[s, pl.ds(start, rows), pl.ds(q, q)].astype(F32)
        g, u = g * scale, u * scale
        hidden = (g / (1.0 + jnp.exp(-g)) * u).astype(BF16)
        hs[pl.ds(start, rows), :] = hidden
        for s in tp_order:
            h_copies[c, s] = send(
                hs.at[pl.ds(start, rows)],
                hr.at[s, pl.ds(start, rows)],
                h_send.at[c, s],
                h_recv.at[c, s],
                {"tp": partner(me_t, s, n_tp)},
            )

    def stage_c(c):
        first, count = chunks[c]
        start, rows = span(c)
        if c == 0:
            loads[8].wait()
        acc = None
        for s in range(n_tp):
            if s > 0:
                h_copies[c, s].wait_recv()
                h = hr[s, pl.ds(start, rows), :]
            else:
                h = hs[pl.ds(start, rows), :]
            p = partner(me_t, s, n_tp)
            term = jnp.dot(h, wd[pl.ds(pl.multiple_of(p * q, q), q), :], preferred_element_type=F32)
            acc = term if acc is None else acc + term
        ob[pl.ds(start, rows), :] = acc.astype(BF16)
        for k in range(first, first + count):
            if k > 0:
                o_copies[k] = send(
                    ob.at[pl.ds(k * cap, cap)],
                    ret.at[pl.ds(k * cap, cap)],
                    o_send.at[k],
                    o_recv.at[k],
                    {"ep": partner(me_e, order[k], n_ep)},
                )

    pl.semaphore_wait(barrier, n_ep - 1 + n_tp - 1)
    dispatch()
    loads[3].wait()
    loads[4].wait()
    stage_a(0)
    for load in loads[5:8]:
        load.wait()
    scores = jnp.exp(score_ref[...])
    weights = prob_ref[...] * scores / jnp.sum(scores, axis=0, keepdims=True)
    slot_col = to_col(slot_row, tok).astype(jnp.int32)
    ids = group_row * per_group + member_ref[...]
    expert_cols = []
    for k in range(n_ep):
        named = jnp.where(ids == partner(me_e, order[k], n_ep), weights, 0.0)
        expert_cols.append(to_col(jnp.sum(named, axis=0, keepdims=True), tok))

    stages = {"a": stage_a, "b": stage_b, "c": stage_c}
    for stage, c in PLAN[1:]:
        stages[stage](c)

    summed = x.astype(F32)
    for k in range(n_ep):
        e = partner(me_e, order[k], n_ep)
        if k > 0:
            o_copies[k].wait_recv()
            rows = ret[pl.ds(k * cap, cap), :]
        else:
            rows = ob[pl.ds(0, cap), :]
        pick = (iota((tok, cap), 1) + (e // per_group) * cap == slot_col).astype(F32).astype(BF16)
        summed = summed + expert_cols[k] * jnp.dot(pick, rows, preferred_element_type=F32)

    square = jnp.sum(summed * summed, axis=1, keepdims=True)
    width = fs.shape[1]
    fs[...] = jnp.broadcast_to(to_row(square, width), (8, width))
    f_copies = {}
    for s in tp_order:
        f_copies[s] = send(fs, fr.at[s], f_send.at[s], f_recv.at[s], {"tp": partner(me_t, s, n_tp)})
    for s in range(1, n_tp):
        f_copies[s].wait_recv()
        square = square + to_col(fr[s][0:1, :], tok)
    out_ref[...] = summed * lax.rsqrt(square / full_width + EPS)

    for copy in pending:
        copy.wait_send()


def solution(mesh):
    n_ep, n_tp = mesh.shape["ep"], mesh.shape["tp"]
    groups = max(2, n_ep // 8)
    order = range(n_ep)
    n_chunks = 4
    each = n_ep // n_chunks
    chunks = tuple((i * each, each) for i in range(n_chunks))

    def local(tokens, group_choice, member_choice, group_prob, member_score, norm_gain, w_gate, w_up, w_down, final_gain):
        tok, dim = tokens.shape
        ff, top = w_gate.shape[2], member_choice.shape[1]
        cap = tok // groups
        q = ff // n_tp
        all_rows = n_ep * cap
        width = -(-max(count * cap for _, count in chunks) // 128) * 128
        out_width = -(-tok // 128) * 128
        vmem = pl.BlockSpec(memory_space=pltpu.VMEM)
        hbm = pl.BlockSpec(memory_space=pltpu.HBM)
        dma = pltpu.SemaphoreType.DMA
        nc = len(chunks)
        normal = pl.pallas_call(
            functools.partial(kernel, (n_ep, n_tp, groups, tuple(order), chunks)),
            out_shape=pltpu.VMEM((tok, dim), F32),
            in_specs=[hbm] * 9,
            out_specs=vmem,
            scratch_shapes=[
                pltpu.VMEM((tok, dim), BF16),
                pltpu.VMEM((1, tok), jnp.int32),
                pltpu.VMEM((top, tok), jnp.int32),
                pltpu.VMEM((1, tok), F32),
                pltpu.VMEM((top, tok), F32),
                pltpu.VMEM((1, dim), F32),
                pltpu.VMEM((dim, ff), BF16),
                pltpu.VMEM((dim, ff), BF16),
                pltpu.VMEM((ff, dim), BF16),
                pltpu.VMEM((tok, dim), BF16),
                pltpu.VMEM((all_rows, dim), BF16),
                pltpu.VMEM((n_tp, all_rows, 2 * q), BF16),
                pltpu.VMEM((n_tp, all_rows, 2 * q), BF16),
                pltpu.VMEM((nc, 8, width), F32),
                pltpu.VMEM((nc, n_tp, 8, width), F32),
                pltpu.VMEM((all_rows, q), BF16),
                pltpu.VMEM((n_tp, all_rows, q), BF16),
                pltpu.VMEM((all_rows, dim), BF16),
                pltpu.VMEM((all_rows, dim), BF16),
                pltpu.VMEM((8, out_width), F32),
                pltpu.VMEM((n_tp, 8, out_width), F32),
                dma((9,)),
                dma((n_ep,)),
                dma((n_ep,)),
                dma((nc, n_tp)),
                dma((nc, n_tp)),
                dma((nc, n_tp)),
                dma((nc, n_tp)),
                dma((nc, n_tp)),
                dma((nc, n_tp)),
                dma((n_ep,)),
                dma((n_ep,)),
                dma((n_tp,)),
                dma((n_tp,)),
            ],
            compiler_params=pltpu.CompilerParams(collective_id=0, has_side_effects=True, vmem_limit_bytes=VMEM_LIMIT),
        )(
            tokens,
            group_choice.reshape(1, tok),
            member_choice.T,
            group_prob.reshape(1, tok),
            member_score.T,
            norm_gain.reshape(1, dim),
            w_gate,
            w_up,
            w_down,
        )
        return (normal * final_gain[None, :]).astype(BF16)

    return jax.shard_map(
        local,
        mesh=mesh,
        in_specs=(
            P(("grp", "ep"), "tp"),
            P(("grp", "ep")),
            P(("grp", "ep"), None),
            P(("grp", "ep")),
            P(("grp", "ep"), None),
            P("tp"),
            P("ep", "tp", None),
            P("ep", "tp", None),
            P("ep", None, "tp"),
            P("tp"),
        ),
        out_specs=P(("grp", "ep"), "tp"),
        check_vma=False,
    )
```
